32 devices in a mesh: kv: 4 (over y, x), tp: 8 (over z, core).
Axes of the slice: x: 2, y: 2, z: 4, core: 2. Of those that a mesh axis runs over, the one named last changes fastest.
Arguments:
- resid: bfloat16 [32, 4096], P('tp', 'kv'), may hold values from -35 to 35
- attn_gain: bfloat16 [4096], replicated, may hold values from 0.099609375 to 1.8984375
- w_query_nope: bfloat16 [4096, 8192], P('kv', 'tp'), may hold values from -0.09375 to 0.09375
- w_query_rope: bfloat16 [4096, 4096], P('kv', 'tp'), may hold values from -0.09375 to 0.09375
- w_latent: bfloat16 [4096, 512], P('kv'), may hold values from -0.09375 to 0.09375
- w_key_rope: bfloat16 [4096, 64], replicated, may hold values from -0.09375 to 0.09375
- latent_gain: bfloat16 [512], replicated, may hold values from 0.099609375 to 1.8984375
- key_up: bfloat16 [512, 64, 128], P(None, 'tp'), may hold values from -0.5 to 0.5
- value_up: bfloat16 [512, 64, 128], P(None, 'tp'), may hold values from -0.25 to 0.25
- w_out: bfloat16 [8192, 4096], P('tp', 'kv'), may hold values from -4 to 4
- post_gain: bfloat16 [4096], replicated, may hold values from 0.099609375 to 1.8984375
- mlp_gain: bfloat16 [4096], replicated, may hold values from 0.099609375 to 1.8984375
- w_gate: bfloat16 [4096, 11008], P('kv', 'tp'), may hold values from -3 to 3
- w_up: bfloat16 [4096, 11008], P('kv', 'tp'), may hold values from -3 to 3
- w_down: bfloat16 [11008, 4096], P('tp', 'kv'), may hold values from -0.0546875 to 0.0546875
- cache_latent: bfloat16 [32, 2048, 512], P('tp', 'kv'), may hold values from -6 to 6
- cache_rope_key: bfloat16 [32, 2048, 64], P('tp', 'kv'), may hold values from -740 to 740
Outputs:
- next_resid: bfloat16 [32, 4096], P('tp', 'kv')
- new_latent: bfloat16 [32, 512], P('tp')
- new_rope_key: bfloat16 [32, 64], P('tp')
The draws below stay inside these ranges and needn't reach their ends.
All inputs are finite; a program needn't handle non-finite values.
Results may differ from the reference program's by a relative error of at most 0.035.
Values may be sent and summed in bfloat16 or wider, within the bound.
A program may use at most 64 MiB of HBM per device.

```python
import jax
import jax.numpy as jnp
from jax import lax

D = 4096
H = 64
NOPE = 128
ROPE = 64
VD = 128
LAT = 512
FF = 11008
POS_DEV = 512
BATCH = 32
CTX = 2048
N_KV = 4


def rising_profile(length, factor):
    place = (jnp.arange(length, dtype=jnp.float32) + 0.5) / length
    profile = jnp.exp(jnp.log(factor) * (place - 0.5))
    return profile / jnp.sqrt(jnp.mean(profile * profile))


def draw_resid(key, part):
    key_base, key_rows = jax.random.split(jax.random.fold_in(key, 101))
    column_pos = jnp.arange(D, dtype=jnp.float32) / D
    column_scale = 0.5 * jnp.exp(jnp.log(4.0) * column_pos)[None, :]
    base_draw = jnp.clip(jax.random.normal(key_base, (BATCH, D), jnp.float32), -6.0, 6.0)
    row_scale = jnp.exp(jax.random.uniform(key_rows, (BATCH, 1), jnp.float32, -0.5, 0.5))
    return (base_draw * column_scale * row_scale).astype(jnp.bfloat16)


def draw_w_out(key, part):
    factor = 6.0
    base_draw = jnp.clip(jax.random.normal(jax.random.fold_in(key, 103), (H * VD, D), jnp.float32), -6.0, 6.0)
    scaled = base_draw * rising_profile(H * VD, factor)[:, None] * rising_profile(D, factor)[None, :]
    return (scaled * (H * VD) ** (-0.5)).astype(jnp.bfloat16)


def rising_rows(key, factor):
    base_draw = jnp.clip(jax.random.normal(key, (D, FF), jnp.float32), -6.0, 6.0)
    return (base_draw * rising_profile(D, factor)[:, None] * D ** (-0.5)).astype(jnp.bfloat16)


def draw_w_gate(key, part):
    factor = 6.0
    return rising_rows(jax.random.fold_in(key, 107), factor)


def draw_w_up(key, part):
    factor = 6.0
    return rising_rows(jax.random.fold_in(key, 109), factor)


def draw_cache_rope_key(key, part):
    key_base = jax.random.fold_in(jax.random.fold_in(key, 113), 0)
    base_draw = jnp.clip(jax.random.normal(key_base, (BATCH, CTX, ROPE), jnp.float32), -6.0, 6.0)
    return base_draw.astype(jnp.bfloat16)


def block_levels(stream_key, shape, cuts, smallest, top_value):
    def one(dim, blocks):
        draws = jax.random.uniform(jax.random.fold_in(jax.random.fold_in(stream_key, 6), dim), (blocks,), jnp.float32, smallest / len(cuts), top_value / len(cuts))
        return jnp.repeat(jnp.exp(draws), shape[dim] // blocks).reshape((-1,) + (1,) * (len(shape) - dim - 1))

    loudness = one(*cuts[0])
    for cut in cuts[1:]:
        loudness = loudness * one(*cut)
    return loudness


def noise(key, shape, width, reach, pieces=(), kind=jnp.bfloat16):
    values = jax.random.normal(key, shape, jnp.float32) * width
    if len(pieces) > 0:
        values = block_levels(key, shape, pieces, -0.22, 0.18) * values
    return jnp.clip(values, min=-reach, max=reach).astype(kind)


def setup_inputs(seed: int = 0) -> dict:
    streams_of = jax.random.split(jax.random.key(seed), 18)
    resid = draw_resid(jax.random.fold_in(streams_of[17], 71), 0)
    attn_gain = jnp.clip(1.0 + 0.18 * jax.random.normal(streams_of[1], (D,), jnp.float32), 0.099609375, 1.8984375).astype(jnp.bfloat16)
    w_query_nope = noise(streams_of[2], (D, H * NOPE), D ** -0.5, 0.09375, ((0, 4), (1, 8)))
    w_query_rope = noise(streams_of[3], (D, H * ROPE), D ** -0.5, 0.09375, ((0, 4), (1, 8)))
    w_latent = noise(streams_of[4], (D, LAT), D ** -0.5, 0.09375, ((0, 4),))
    w_key_rope = noise(streams_of[5], (D, ROPE), D ** -0.5, 0.09375)
    latent_gain = jnp.clip(1.0 + 0.18 * jax.random.normal(streams_of[6], (LAT,), jnp.float32), 0.099609375, 1.8984375).astype(jnp.bfloat16)
    key_up = noise(streams_of[7], (LAT, H, NOPE), NOPE ** -0.5, 0.5, ((1, 8),))
    value_up = noise(streams_of[8], (LAT, H, VD), LAT ** -0.5, 0.25, ((1, 8),))
    w_out = draw_w_out(jax.random.fold_in(streams_of[17], 71), 0)
    post_gain = jnp.clip(1.0 + 0.18 * jax.random.normal(streams_of[10], (D,), jnp.float32), 0.099609375, 1.8984375).astype(jnp.bfloat16)
    mlp_gain = jnp.clip(1.0 + 0.18 * jax.random.normal(streams_of[11], (D,), jnp.float32), 0.099609375, 1.8984375).astype(jnp.bfloat16)
    w_gate = draw_w_gate(jax.random.fold_in(streams_of[17], 71), 0)
    w_up = draw_w_up(jax.random.fold_in(streams_of[17], 71), 0)
    w_down = noise(streams_of[14], (FF, D), FF ** -0.5, 0.0546875, ((0, 8), (1, 4)))
    cache_latent = noise(streams_of[15], (BATCH, CTX, LAT), 1.0, 6.0, ((0, 8), (1, 4)))
    cache_rope_key = draw_cache_rope_key(jax.random.fold_in(streams_of[17], 71), 0)
    return dict(resid=resid, attn_gain=attn_gain, w_query_nope=w_query_nope, w_query_rope=w_query_rope, w_latent=w_latent, w_key_rope=w_key_rope, latent_gain=latent_gain, key_up=key_up, value_up=value_up, w_out=w_out, post_gain=post_gain, mlp_gain=mlp_gain, w_gate=w_gate, w_up=w_up, w_down=w_down, cache_latent=cache_latent, cache_rope_key=cache_rope_key)


EPS = 1e-06
THETA = 10000.0

def rotate(vector, position):
    half_width = vector.shape[-1] // 2
    frequency = THETA ** (-jnp.arange(half_width, dtype=jnp.float32) / half_width)
    angles = jnp.asarray(position, jnp.float32) * frequency
    cos_table, sin_table = (jnp.cos(angles), jnp.sin(angles))
    lower_half, upper_half = (vector[..., :half_width], vector[..., half_width:])
    return jnp.concatenate([lower_half * cos_table - upper_half * sin_table, lower_half * sin_table + upper_half * cos_table], axis=-1)

def reference(resid, attn_gain, w_query_nope, w_query_rope, w_latent, w_key_rope, latent_gain, key_up, value_up, w_out, post_gain, mlp_gain, w_gate, w_up, w_down, cache_latent, cache_rope_key):
    batch_rows = resid.shape[0]
    head_count = key_up.shape[1]
    context = cache_latent.shape[1]
    latent_width = cache_latent.shape[2]
    score_scale = (key_up.shape[2] + cache_rope_key.shape[2]) ** (-0.5)
    resid_float = resid.astype(jnp.float32)
    normed_a = (resid_float * attn_gain.astype(jnp.float32)).astype(jnp.bfloat16)
    scale_in = lax.rsqrt(lax.optimization_barrier(jnp.mean(resid_float * resid_float, axis=1, keepdims=True)) + EPS)
    q_nope = (jnp.dot(normed_a, w_query_nope, preferred_element_type=jnp.float32) * scale_in).astype(jnp.bfloat16)
    q_rope_raw = jnp.dot(normed_a, w_query_rope, preferred_element_type=jnp.float32) * scale_in
    q_rope = rotate(q_rope_raw.reshape(batch_rows, head_count, -1), context).astype(jnp.bfloat16)
    latent_raw = jnp.dot(normed_a, w_latent, preferred_element_type=jnp.float32)
    new_latent = (latent_raw * lax.rsqrt(lax.optimization_barrier(jnp.mean(latent_raw * latent_raw, axis=1, keepdims=True)) + EPS) * latent_gain.astype(jnp.float32)).astype(jnp.bfloat16)
    key_raw = jnp.dot(normed_a, w_key_rope, preferred_element_type=jnp.float32) * scale_in
    new_rope_key = rotate(key_raw, context).astype(jnp.bfloat16)
    q_lat = jnp.einsum('bhd,chd->bhc', q_nope.reshape(batch_rows, head_count, -1).astype(jnp.float32), key_up.astype(jnp.float32)).astype(jnp.bfloat16)

    def attend(item):
        query_lat, query_rope, keys, rope_keys, own_latent, own_rope = item
        scores = (jnp.dot(query_lat, keys.T, preferred_element_type=jnp.float32) + jnp.dot(query_rope, rope_keys.T, preferred_element_type=jnp.float32)) * score_scale
        own_score = (jnp.dot(query_lat, own_latent, preferred_element_type=jnp.float32) + jnp.dot(query_rope, own_rope, preferred_element_type=jnp.float32)) * score_scale
        peak = jnp.maximum(lax.optimization_barrier(jnp.max(scores, axis=1)), own_score)
        probs = jnp.exp(scores - peak[:, None])
        own_prob = jnp.exp(own_score - peak)
        totals = lax.optimization_barrier(jnp.sum(probs, axis=1)) + own_prob
        weights = probs.astype(jnp.bfloat16).reshape(head_count, N_KV, POS_DEV)
        blocks = keys.reshape(N_KV, POS_DEV, latent_width)
        partial_value = jnp.einsum('hjp,jpc->hjc', weights.astype(jnp.float32), blocks.astype(jnp.float32))
        partial_value = partial_value.astype(jnp.bfloat16).astype(jnp.float32)
        summed = lax.optimization_barrier(jnp.sum(partial_value, axis=1)) + own_prob[:, None] * own_latent.astype(jnp.float32)[None, :]
        return (summed / totals[:, None]).astype(jnp.bfloat16)
    o_lat = lax.map(attend, (q_lat, q_rope, cache_latent, cache_rope_key, new_latent, new_rope_key))
    o_heads = jnp.einsum('bhc,che->bhe', o_lat.astype(jnp.float32), value_up.astype(jnp.float32))
    o_heads = o_heads.astype(jnp.bfloat16).reshape(batch_rows, -1)
    attended = jnp.dot(o_heads, w_out, preferred_element_type=jnp.float32)
    post_part = attended * lax.rsqrt(lax.optimization_barrier(jnp.mean(attended * attended, axis=1, keepdims=True)) + EPS) * post_gain.astype(jnp.float32)
    resid_mid = (resid_float + post_part).astype(jnp.bfloat16)
    mid_float = resid_mid.astype(jnp.float32)
    normed_m = (mid_float * mlp_gain.astype(jnp.float32)).astype(jnp.bfloat16)
    scale_mid = lax.rsqrt(lax.optimization_barrier(jnp.mean(mid_float * mid_float, axis=1, keepdims=True)) + EPS)
    gate = jnp.dot(normed_m, w_gate, preferred_element_type=jnp.float32) * scale_mid
    up_part = jnp.dot(normed_m, w_up, preferred_element_type=jnp.float32) * scale_mid
    hidden = (jax.nn.silu(gate) * up_part).astype(jnp.bfloat16)
    next_resid = (mid_float + jnp.dot(hidden, w_down, preferred_element_type=jnp.float32)).astype(jnp.bfloat16)
    return (next_resid, new_latent, new_rope_key)
```

```python
import functools

import jax
import jax.numpy as jnp
import numpy as np
from jax import lax
from jax.experimental import pallas as pl
from jax.experimental.pallas import tpu as pltpu
from jax.sharding import PartitionSpec as P

EPS = 1e-06
THETA = 10000.0


def rotate(vector, position):
    half_width = vector.shape[-1] // 2
    frequency = THETA ** (-jnp.arange(half_width, dtype=jnp.float32) / half_width)
    angles = jnp.asarray(position, jnp.float32) * frequency
    cos_table, sin_table = (jnp.cos(angles), jnp.sin(angles))
    lower_half, upper_half = (vector[..., :half_width], vector[..., half_width:])
    return jnp.concatenate(
        [
            lower_half * cos_table - upper_half * sin_table,
            lower_half * sin_table + upper_half * cos_table,
        ],
        axis=-1,
    )


def body(
    resid,
    attn_gain,
    w_query_nope,
    w_query_rope,
    w_latent,
    w_key_rope,
    latent_gain,
    key_up,
    value_up,
    w_out,
    post_gain,
    mlp_gain,
    w_gate,
    w_up,
    w_down,
    cache_latent,
    cache_rope_key,
):
    kv_count = lax.axis_size("kv")
    kv_index = lax.axis_index("kv")
    tp_index = lax.axis_index("tp")
    own_rows, width_dev = resid.shape
    model_width = width_dev * kv_count
    heads_dev = key_up.shape[1]
    pos_dev = cache_latent.shape[1]
    context = pos_dev * kv_count
    score_scale = (key_up.shape[2] + cache_rope_key.shape[2]) ** (-0.5)
    col_start = kv_index * width_dev
    row_start = tp_index * own_rows

    def block_of(vector):
        return lax.dynamic_slice_in_dim(vector, col_start, width_dev, 0).astype(jnp.float32)[
            None, :
        ]

    gathered = lax.all_gather(resid, "tp", axis=0, tiled=True)
    batch_rows = gathered.shape[0]
    gathered_float = gathered.astype(jnp.float32)
    normed_a = (gathered_float * block_of(attn_gain)).astype(jnp.bfloat16)
    own_normed = lax.dynamic_slice_in_dim(normed_a, row_start, own_rows, 0)
    key_rows = lax.dynamic_slice_in_dim(w_key_rope, col_start, width_dev, 0)
    q_nope_sum, q_rope_sum, latent_sum, key_sum, square_sum = (
        lax.psum(
            jnp.dot(normed_a, w_query_nope, preferred_element_type=jnp.float32).astype(
                jnp.bfloat16
            ),
            "kv",
        ).astype(jnp.float32),
        lax.psum(
            jnp.dot(normed_a, w_query_rope, preferred_element_type=jnp.float32).astype(
                jnp.bfloat16
            ),
            "kv",
        ).astype(jnp.float32),
        lax.psum(
            jnp.dot(own_normed, w_latent, preferred_element_type=jnp.float32).astype(jnp.bfloat16),
            "kv",
        ).astype(jnp.float32),
        lax.psum(
            jnp.dot(own_normed, key_rows, preferred_element_type=jnp.float32).astype(jnp.bfloat16),
            "kv",
        ).astype(jnp.float32),
        lax.psum(
            jnp.sum(gathered_float * gathered_float, axis=1).astype(jnp.bfloat16), "kv"
        ).astype(jnp.float32),
    )
    scale_in = lax.rsqrt(square_sum / model_width + EPS)[:, None]
    own_scale = lax.dynamic_slice_in_dim(scale_in, row_start, own_rows, 0)
    q_nope = (q_nope_sum * scale_in).astype(jnp.bfloat16).reshape(batch_rows, heads_dev, -1)
    q_rope = rotate((q_rope_sum * scale_in).reshape(batch_rows, heads_dev, -1), context).astype(
        jnp.bfloat16
    )
    new_latent = (
        latent_sum
        * lax.rsqrt(jnp.mean(latent_sum * latent_sum, axis=1, keepdims=True) + EPS)
        * latent_gain.astype(jnp.float32)[None, :]
    ).astype(jnp.bfloat16)
    new_rope_key = rotate(key_sum * own_scale, context).astype(jnp.bfloat16)
    q_lat = jnp.einsum("bhd,chd->bhc", q_nope, key_up, preferred_element_type=jnp.float32).astype(
        jnp.bfloat16
    )
    seq_lat, seq_rope = (
        lax.all_to_all(q_lat, "tp", split_axis=0, concat_axis=1, tiled=True),
        lax.all_to_all(q_rope, "tp", split_axis=0, concat_axis=1, tiled=True),
    )
    scores = (
        jnp.einsum("bhc,bpc->bhp", seq_lat, cache_latent, preferred_element_type=jnp.float32)
        + jnp.einsum("bhr,bpr->bhp", seq_rope, cache_rope_key, preferred_element_type=jnp.float32)
    ) * score_scale
    own_score = (
        jnp.einsum("bhc,bc->bh", seq_lat, new_latent, preferred_element_type=jnp.float32)
        + jnp.einsum("bhr,br->bh", seq_rope, new_rope_key, preferred_element_type=jnp.float32)
    ) * score_scale
    local_peak = jnp.maximum(jnp.max(scores, axis=2), own_score)
    peak = lax.pmax(local_peak, "kv")
    probs = jnp.exp(scores - peak[:, :, None])
    own_prob = jnp.exp(own_score - peak)
    totals = lax.psum(jnp.sum(probs, axis=2), "kv") + own_prob
    partial_value = jnp.einsum(
        "bhp,bpc->bhc", probs.astype(jnp.bfloat16), cache_latent, preferred_element_type=jnp.float32
    )
    summed = (
        lax.psum(partial_value.astype(jnp.bfloat16), "kv").astype(jnp.float32)
        + own_prob[:, :, None] * new_latent.astype(jnp.float32)[:, None, :]
    )
    o_lat = (summed / totals[:, :, None]).astype(jnp.bfloat16)
    head_lat = lax.all_to_all(o_lat, "tp", split_axis=1, concat_axis=0, tiled=True)
    o_heads = jnp.einsum(
        "bhc,che->bhe", head_lat, value_up, preferred_element_type=jnp.float32
    ).astype(jnp.bfloat16)
    o_flat = o_heads.reshape(batch_rows, -1)
    attended = lax.psum_scatter(
        jnp.dot(o_flat, w_out, preferred_element_type=jnp.float32).astype(jnp.bfloat16),
        "tp",
        scatter_dimension=0,
        tiled=True,
    ).astype(jnp.float32)
    post_square = lax.psum(jnp.sum(attended * attended, axis=1), "kv")
    post_part = attended * lax.rsqrt(post_square / model_width + EPS)[:, None] * block_of(post_gain)
    resid_mid = (resid.astype(jnp.float32) + post_part).astype(jnp.bfloat16)
    mid_rows = lax.all_gather(resid_mid, "tp", axis=0, tiled=True)
    mid_float = mid_rows.astype(jnp.float32)
    normed_m = (mid_float * block_of(mlp_gain)).astype(jnp.bfloat16)
    gate_part = jnp.dot(normed_m, w_gate, preferred_element_type=jnp.float32)
    up_part = jnp.dot(normed_m, w_up, preferred_element_type=jnp.float32)
    square_part = jnp.sum(mid_float * mid_float, axis=1)
    gate_sum, up_sum, mid_square = (
        lax.psum(gate_part.astype(jnp.bfloat16), "kv").astype(jnp.float32),
        lax.psum(up_part.astype(jnp.bfloat16), "kv").astype(jnp.float32),
        lax.psum(square_part.astype(jnp.bfloat16), "kv").astype(jnp.float32),
    )
    scale_mid = lax.rsqrt(mid_square / model_width + EPS)[:, None]
    hidden = (jax.nn.silu(gate_sum * scale_mid) * (up_sum * scale_mid)).astype(jnp.bfloat16)
    lowered = lax.psum_scatter(
        jnp.dot(hidden, w_down, preferred_element_type=jnp.float32).astype(jnp.bfloat16),
        "tp",
        scatter_dimension=0,
        tiled=True,
    ).astype(jnp.float32)
    next_resid = (resid_mid.astype(jnp.float32) + lowered).astype(jnp.bfloat16)
    return (next_resid, new_latent, new_rope_key)


F32 = jnp.float32
BF16 = jnp.bfloat16
MESH = pl.DeviceIdType.MESH


def dot_nt(a, b):
    return lax.dot_general(a, b, (((1,), (1,)), ((), ())), preferred_element_type=F32)


def lane_iota(shape):
    return lax.broadcasted_iota(jnp.int32, shape, len(shape) - 1)


def turn(v, cos, sin, half):
    width = v.shape[-1]
    low = lane_iota(v.shape) % (2 * half) < half
    swapped = jnp.where(low, pltpu.roll(v, width - half, 1), pltpu.roll(v, half, 1))
    return v * cos + swapped * sin


def flip(i, mask):
    out, bit = i, 1
    while bit <= mask:
        if mask & bit:
            out = out + bit - 2 * bit * lax.rem(lax.div(i, bit), 2)
        bit *= 2
    return out


PHASES = ("x", "lat", "q", "sq", "qe", "rel", "acc", "ml", "o", "early", "h", "es", "ab", "gu", "sm", "hb", "ps", "ls")


def layer_kernel(
    K, T,
    h_x, h_ag, h_lg, h_pg, h_mg, h_cos, h_sin,
    h_wqn, h_wqr, h_wlat, h_wkr, h_ku, h_vu, h_wo, h_wg, h_wu, h_wd, h_cl, h_cr,
    out, out_lat, out_key,
    ag, lg, pg, mg, cos_ref, sin_ref,
    wqn, wqr, wlat, wkr, ku, vu, wo, wg, wu, wd, cl, cr,
    xbuf, xf, qs, qrv, sqs, sqr, lats, latr, qe, qbuf, accs, accr, mls, mlr,
    nls, nks, osend, obuf, ohs, h3, es, er, ab, attf, tall,
    eas, ear, easum, gus, gur, sms, smr, hb, psb, ls, lr, wide_ref, kus, vus,
    lsem, ssem, rsem, qsem, relsem,
):
    k = lax.axis_index("kv")
    t = lax.axis_index("tp")
    _, R, W = xbuf.shape
    D = W * K
    B = R * T
    LAT = h_wlat.shape[1]
    ROPE = h_wkr.shape[0]
    QN = h_wqn.shape[1]
    QR = h_wqr.shape[1]
    HD = QR // ROPE
    NOPE = QN // HD
    H = HD * T
    VD = h_vu.shape[1]
    half = ROPE // 2
    score_scale = (NOPE + ROPE) ** (-0.5)
    col = pl.ds(pl.multiple_of(k * W, 128), W)
    gain_rows = pl.ds(pl.multiple_of(k * (W // 128), W // 128), W // 128)

    z, core = lax.div(t, 2), lax.rem(t, 2)
    middle = lax.rem(lax.div(z + 1, 2), 2)
    two, end = lax.rem(z + 2, 4), 3 - z
    far = middle * two + (1 - middle) * end
    mid = middle * end + (1 - middle) * two
    near = flip(z, 1)
    by_arrival = [flip(t, 1)] + [2 * zz + cc for zz in (near, mid, far) for cc in (core, 1 - core)]
    tps = by_arrival[::-1]
    kvs = [flip(k, m) for m in (3, 1, 2)]

    barrier = pltpu.get_barrier_semaphore()
    for kk, tt in [(kk, t) for kk in kvs] + [(k, tt) for tt in tps]:
        pl.semaphore_signal(barrier, inc=1, device_id=(kk, tt), device_id_type=MESH)

    loads = {}
    pairs = [
        ("x", h_x, xbuf.at[t]), ("ag", h_ag.at[gain_rows], ag), ("lat", h_wlat, wlat),
        ("kr", h_wkr.at[:, col], wkr), ("ku", h_ku, ku), ("qn", h_wqn, wqn), ("qr", h_wqr, wqr),
        ("lg", h_lg, lg), ("cos", h_cos, cos_ref), ("sin", h_sin, sin_ref),
        ("vu", h_vu, vu), ("cl", h_cl, cl), ("cr", h_cr, cr),
        ("mg", h_mg.at[gain_rows], mg), ("pg", h_pg.at[gain_rows], pg),
        ("wg", h_wg, wg), ("wu", h_wu, wu), ("wo", h_wo, wo), ("wd", h_wd, wd),
    ]
    for i, (name, src, dst) in enumerate(pairs):
        loads[name] = pltpu.make_async_copy(src, dst, lsem.at[i])
        loads[name].start()

    def send(phase, src, dst, to, landed=None):
        i = PHASES.index(phase)
        pltpu.make_async_remote_copy(
            src_ref=src, dst_ref=dst, send_sem=ssem.at[i],
            recv_sem=rsem.at[i] if landed is None else landed,
            device_id=to, device_id_type=MESH,
        ).start()

    def settle(ref, sem):
        pltpu.make_async_remote_copy(
            src_ref=ref, dst_ref=ref, send_sem=sem, recv_sem=sem,
            device_id=(k, tps[-1]), device_id_type=MESH,
        ).wait_recv()

    def arrive(phase, ref):
        settle(ref, rsem.at[PHASES.index(phase)])

    def left(phase, ref):
        settle(ref, ssem.at[PHASES.index(phase)])

    def dot(a, b):
        return jnp.dot(a, b[...], preferred_element_type=F32)

    def put_rows(ref, s, v):
        for c in range(ref.shape[0]):
            ref[c, pl.ds(s, R, stride=T), :] = v[:, c * 128:(c + 1) * 128]

    def rows(ref, s):
        return jnp.concatenate(
            [ref[c, pl.ds(s, R, stride=T), :] for c in range(ref.shape[0])], axis=1
        )

    def put_all(ref, v):
        for c in range(ref.shape[0]):
            ref[c] = v[:, c * 128:(c + 1) * 128]

    def all_rows(ref):
        return jnp.concatenate([ref[c] for c in range(ref.shape[0])], axis=1)

    def gain_row(ref):
        g = ref[...].astype(F32)
        return jnp.concatenate([g[i:i + 1] for i in range(g.shape[0])], axis=1)

    def by_head(src, dst):
        n = src.shape[1]
        wide_ref[...] = src[...].astype(F32)
        for h in range(HD):
            dst[:, h * n:(h + 1) * n] = wide_ref[pl.ds(h, LAT, stride=HD), :].astype(BF16)

    loads["x"].wait()
    pl.semaphore_wait(barrier, len(tps) + len(kvs))
    for tt in tps:
        send("x", xbuf.at[t], xbuf.at[t], (k, tt))
    xo = xbuf[pl.ds(t, 1)][0].astype(F32)
    loads["ag"].wait()
    again = gain_row(ag)
    own_normed = (xo * again).astype(BF16)
    loads["lat"].wait()
    loads["kr"].wait()
    lats[:, :LAT] = dot(own_normed, wlat)
    lats[:, LAT:LAT + ROPE] = dot_nt(own_normed, wkr[...])
    lats[:, LAT + ROPE:] = jnp.broadcast_to(
        jnp.sum(xo * xo, axis=1, keepdims=True), (R, lats.shape[1] - LAT - ROPE)
    )
    latr[pl.ds(k, 1)] = lats[...][None]
    for kk in kvs:
        send("lat", lats, latr.at[k], (kk, t))
    loads["ku"].wait()
    by_head(ku, kus)
    arrive("x", xbuf.at[pl.ds(0, T - 1)])
    for s in range(T):
        put_rows(xf, s, xbuf[s].astype(F32))
    x = all_rows(xf)
    normed = (x * again).astype(BF16)
    sqs[...] = jnp.broadcast_to(jnp.sum(x * x, axis=1, keepdims=True), (B, 128)).reshape(K, T, 128)
    loads["qn"].wait()
    qs[:, :, :QN] = dot(normed, wqn).reshape(K, T, QN).astype(BF16)
    loads["qr"].wait()
    qs[:, :, QN:] = dot(normed, wqr).reshape(K, T, QR).astype(BF16)
    for kk in kvs:
        send("q", qs.at[kk], qrv.at[k], (kk, t))
        send("sq", sqs.at[kk], sqr.at[k], (kk, t))
    qrv[pl.ds(k, 1)] = qs[pl.ds(k, 1)]
    sqr[pl.ds(k, 1)] = sqs[pl.ds(k, 1)]
    loads["vu"].wait()
    by_head(vu, vus)
    for name in ("lg", "cos", "sin"):
        loads[name].wait()
    arrive("lat", latr.at[pl.ds(0, K - 1)])
    lat = sum(latr[s] for s in range(K))
    raw = lat[:, :LAT]
    new_lat = (
        raw * lax.rsqrt(jnp.mean(raw * raw, axis=1, keepdims=True) + EPS) * gain_row(lg)
    ).astype(BF16)
    own_scale = lax.rsqrt(lat[:, LAT + ROPE:LAT + ROPE + 1] / D + EPS)
    tail = lat[:, LAT:]
    turned = turn(tail * own_scale, cos_ref[:, :tail.shape[1]], sin_ref[:, :tail.shape[1]], half)
    new_key = jnp.where(lane_iota(turned.shape) < ROPE, turned, 0.0).astype(BF16)
    out_lat[...] = new_lat
    out_key[...] = new_key[:, :ROPE]
    nls[...] = new_lat.astype(F32)
    nks[...] = new_key.astype(F32)

    arrive("q", qrv.at[pl.ds(0, K - 1)])
    arrive("sq", sqr.at[pl.ds(0, K - 1)])
    q = sum(qrv[s].astype(F32) for s in range(K))
    square = sum(sqr[s] for s in range(K))[:, :1]
    scale = lax.rsqrt(square / D + EPS)
    q_nope = (q[:, :QN] * scale).astype(BF16).astype(F32)
    q_rope = turn(q[:, QN:] * scale, cos_ref[...], sin_ref[...], half).astype(BF16).astype(F32)

    def own_head(width, each):
        shape = (HD, width)
        return lane_iota(shape) // each == lax.broadcasted_iota(jnp.int32, shape, 0)

    def spread(v, each):
        mask = own_head(v.shape[1], each)
        return jnp.concatenate(
            [jnp.where(mask, jnp.broadcast_to(v[i:i + 1], mask.shape), 0.0) for i in range(T)], axis=0
        ).astype(BF16)

    RP = qe.shape[2] - LAT
    fold_shape = (QR, RP)
    fold = (
        lax.broadcasted_iota(jnp.int32, fold_shape, 0) % ROPE == lane_iota(fold_shape)
    ).astype(F32).astype(BF16)
    qe[:, :, LAT:] = jnp.dot(
        spread(q_rope, ROPE), fold, preferred_element_type=F32
    ).reshape(T, HD, RP).astype(BF16)
    qe[:, :, :LAT] = dot_nt(spread(q_nope, NOPE), kus[...]).reshape(T, HD, LAT).astype(BF16)
    for tt in tps:
        send("qe", qe.at[tt], qbuf.at[k, t], (k, tt), qsem.at[t])
    for i, kk in enumerate(kvs):
        send("rel", qe.at[t], qbuf.at[k, t], (kk, t), relsem.at[i])
    qbuf[pl.ds(k, 1), pl.ds(t, 1)] = qe[pl.ds(t, 1)][None]
    for tt in by_arrival:
        slot = qbuf.at[k, tt]
        settle(slot, qsem.at[tt])
        for i, kk in enumerate(kvs):
            send("rel", slot, slot, (kk, t), relsem.at[i])
    loads["cl"].wait()
    loads["cr"].wait()

    def attend(b):
        qb32 = qbuf[pl.ds(b, 1)][0].astype(F32).reshape(H, LAT + RP)
        qb = qb32.astype(BF16)
        keys = cl[pl.ds(b, 1)][0]
        scores = (
            dot_nt(qb[:, :LAT], keys) + jnp.dot(
                qb[:, LAT:LAT + ROPE], cr[pl.ds(b, 1)][0], preferred_element_type=F32
            )
        ) * score_scale
        m = jnp.max(scores, axis=1, keepdims=True)
        p = jnp.exp(scores - m)
        total = jnp.sum(p, axis=1, keepdims=True)
        acc = jnp.dot(p.astype(BF16), keys, preferred_element_type=F32).astype(BF16)
        turned_ml = jnp.where(lane_iota((H, 2 * H)) < H, m, total).T
        return qb32, acc, turned_ml[:1], turned_ml[H:H + 1]

    own_qb, acc, m_row, total_row = attend(k)
    accr[pl.ds(k, 1)] = acc[None]
    mlr[pl.ds(k, 1), 0:1, :H] = m_row[None]
    mlr[pl.ds(k, 1), 1:2, :H] = total_row[None]
    nl = nls[pl.ds(k, 1), :]
    nk = nks[pl.ds(k, 1), :]
    own_score = (
        jnp.sum(own_qb[:, :LAT] * nl, axis=1, keepdims=True)
        + jnp.sum(own_qb[:, LAT:] * nk, axis=1, keepdims=True)
    ) * score_scale
    for i, kk in ((1, kvs[1]), (2, kvs[2]), (0, kvs[0])):
        settle(qbuf.at[kk], relsem.at[i])
        _, acc, m_row, total_row = attend(kk)
        mls[i, 0:1, :H] = m_row
        mls[i, 1:2, :H] = total_row
        accs[i] = acc
        send("acc", accs.at[i], accr.at[k], (kk, t))
        send("ml", mls.at[i], mlr.at[k], (kk, t))
    arrive("ml", mlr.at[pl.ds(0, K - 1)])
    arrive("acc", accr.at[pl.ds(0, K - 1)])
    columns = mlr[...].reshape(K * mlr.shape[1], mlr.shape[2]).T[:H]
    peaks = [columns[:, 8 * s:8 * s + 1] for s in range(K)]
    peak = own_score
    for m in peaks:
        peak = jnp.maximum(peak, m)
    own_prob = jnp.exp(own_score - peak)
    total = own_prob
    summed = own_prob * nl
    for s in range(K):
        w = jnp.exp(peaks[s] - peak)
        total = total + w * columns[:, 8 * s + 1:8 * s + 2]
        summed = summed + w * accr[s].astype(F32)
    osend[...] = (summed / total).reshape(T, HD, LAT).astype(BF16)
    for tt in tps:
        send("o", osend.at[tt], obuf.at[t], (k, tt))
    obuf[pl.ds(t, 1)] = osend[pl.ds(t, 1)]

    FD = wg.shape[0]
    loads["mg"].wait()
    early = (all_rows(xf) * gain_row(mg)).astype(BF16)
    for i, (name, w) in enumerate((("wg", wg), ("wu", wu))):
        loads[name].wait()
        eas[:, i] = dot_nt(early, w[...]).reshape(K, T, FD).astype(BF16)
        for kk in kvs:
            send("early", eas.at[kk, i], ear.at[k, i], (kk, t))
    ear[pl.ds(k, 1)] = eas[pl.ds(k, 1)]
    arrive("o", obuf.at[pl.ds(0, T - 1)])
    wide = dot(obuf[...].astype(F32).reshape(T * HD, LAT).astype(BF16), vus)
    mask = own_head(HD * VD, VD)
    for i in range(T):
        ohs[i:i + 1, :] = jnp.sum(
            jnp.where(mask, wide[i * HD:(i + 1) * HD], 0.0), axis=0, keepdims=True
        )
    h3[pl.ds(k, 1)] = ohs[...].astype(BF16)[None]
    for kk in kvs:
        send("h", h3.at[k], h3.at[k], (kk, t))
    loads["wo"].wait()
    arrive("h", h3.at[pl.ds(0, K - 1)])
    es[...] = dot(h3[...].astype(F32).reshape(B, HD * VD).astype(BF16), wo).reshape(K, T, W).astype(BF16)
    first = (T - K) // 2
    mine = t - first
    owner = jnp.logical_and(mine >= 0, mine < K)
    for i in range(K):
        j = lax.rem(i + (K // 2) * (1 - lax.div(t, T // 2)), K)

        @pl.when(mine != j)
        def _():
            send("es", es.at[j], er.at[t], (k, first + j))

    arrive("early", ear.at[pl.ds(0, K - 1)])
    easum[...] = sum(ear[s].astype(F32) for s in range(K))
    loads["pg"].wait()

    @pl.when(owner)
    def _():
        er[pl.ds(t, 1)] = es[pl.ds(mine, 1)]
        arrive("es", er.at[pl.ds(0, T - 1)])
        ab[pl.ds(mine, 1)] = sum(er[s].astype(F32) for s in range(T)).astype(BF16)[None]
        for tt in tps:
            send("ab", ab.at[mine], ab.at[mine], (k, tt))
        arrive("ab", ab.at[pl.ds(0, K - 1)])

    @pl.when(jnp.logical_not(owner))
    def _():
        arrive("ab", ab)

    att = ab[...].astype(F32).reshape(B, W)
    added = att * gain_row(pg)
    late = (added * gain_row(mg)).astype(BF16)
    gus[:, 0] = dot_nt(late, wg[...]).reshape(K, T, FD).astype(BF16)
    for kk in kvs:
        send("gu", gus.at[kk, 0], gur.at[k, 0], (kk, t))
    gus[:, 1] = dot_nt(late, wu[...]).reshape(K, T, FD).astype(BF16)
    for kk in kvs:
        send("gu", gus.at[kk, 1], gur.at[k, 1], (kk, t))
    lane = lane_iota((B, 128))
    parts = (
        jnp.sum(att * att, axis=1, keepdims=True),
        jnp.sum(all_rows(xf) * added, axis=1, keepdims=True),
        jnp.sum(added * added, axis=1, keepdims=True),
    )
    sms[...] = jnp.where(
        lane < 32, parts[0], jnp.where(lane < 64, parts[1], parts[2])
    ).reshape(K, T, 128)
    for kk in kvs:
        send("sm", sms.at[kk], smr.at[k], (kk, t))
    gur[pl.ds(k, 1)] = gus[pl.ds(k, 1)]
    smr[pl.ds(k, 1)] = sms[pl.ds(k, 1)]
    put_all(attf, att)
    arrive("sm", smr.at[pl.ds(0, K - 1)])
    arrive("gu", gur.at[pl.ds(0, K - 1)])
    sums = sum(smr[s] for s in range(K))
    post_scale = lax.rsqrt(sums[:, :1] / D + EPS)
    mid_square = square + post_scale * (2.0 * sums[:, 32:33] + post_scale * sums[:, 64:65])
    mid_scale = lax.rsqrt(jnp.maximum(mid_square, 0.0) / D + EPS)
    gate = (easum[0] + post_scale * sum(gur[s, 0].astype(F32) for s in range(K))) * mid_scale
    up = (easum[1] + post_scale * sum(gur[s, 1].astype(F32) for s in range(K))) * mid_scale
    hb[pl.ds(k, 1)] = (gate / (1.0 + jnp.exp(-gate)) * up).astype(BF16)[None]
    psb[pl.ds(k, 1)] = jnp.broadcast_to(post_scale, (T, 128))[None]
    for kk in kvs:
        send("hb", hb.at[k], hb.at[k], (kk, t))
        send("ps", psb.at[k], psb.at[k], (kk, t))
    loads["wd"].wait()
    arrive("hb", hb.at[pl.ds(0, K - 1)])
    put_all(tall, dot(hb[...].astype(F32).reshape(B, FD).astype(BF16), wd))
    for s in range(T):
        ls[s] = rows(tall, s).astype(BF16)
    for tt in tps:
        send("ls", ls.at[tt], lr.at[t], (k, tt))
    lr[pl.ds(t, 1)] = ls[pl.ds(t, 1)]
    arrive("ps", psb.at[pl.ds(0, K - 1)])
    own_post = psb[:, pl.ds(t, 1), :].reshape(K, 128)[:, :1]
    mid_own = (
        xbuf[pl.ds(t, 1)][0].astype(F32) + rows(attf, t) * own_post * gain_row(pg)
    ).astype(BF16).astype(F32)
    left("x", xbuf.at[pl.ds(0, T - 1)])
    left("lat", latr.at[pl.ds(0, K - 1)])
    left("q", qs.at[pl.ds(0, K - 1)])
    left("sq", sqs.at[pl.ds(0, K - 1)])
    left("qe", qe.at[pl.ds(0, T - 1)])
    left("rel", qbuf.at[pl.ds(0, K - 1)])
    left("acc", accs)
    left("ml", mls)
    left("o", osend.at[pl.ds(0, T - 1)])
    left("early", eas.at[pl.ds(0, K - 1)])
    left("h", h3.at[pl.ds(0, K - 1)])

    @pl.when(owner)
    def _():
        left("es", es.at[pl.ds(0, K - 1)])
        left("ab", er.at[pl.ds(0, T - 1)])

    @pl.when(jnp.logical_not(owner))
    def _():
        left("es", es)

    left("gu", gus.at[pl.ds(0, K - 1)])
    left("sm", sms.at[pl.ds(0, K - 1)])
    left("hb", hb.at[pl.ds(0, K - 1)])
    left("ps", psb.at[pl.ds(0, K - 1)])
    arrive("ls", lr.at[pl.ds(0, T - 1)])
    lowered = sum(lr[s].astype(F32) for s in range(T))
    out[...] = (mid_own + lowered).astype(BF16)
    left("ls", ls.at[pl.ds(0, T - 1)])


def hand_over(a, b, c, a_out, b_out, c_out):
    for src, dst in ((a, a_out), (b, b_out), (c, c_out)):
        dst[...] = src[...]


def fused(
    resid, attn_gain, w_query_nope, w_query_rope, w_latent, w_key_rope, latent_gain, key_up,
    value_up, w_out, post_gain, mlp_gain, w_gate, w_up, w_down, cache_latent, cache_rope_key,
):
    K = lax.axis_size("kv")
    T = lax.axis_size("tp")
    R, W = resid.shape
    LAT, HD, _ = key_up.shape
    key_flat = key_up.reshape(LAT * HD, -1)
    value_flat = value_up.reshape(LAT * HD, -1)
    key_turned, rope_turned = w_key_rope.T, jnp.swapaxes(cache_rope_key, 1, 2)
    gate_turned, up_turned = w_gate.T, w_up.T
    ROPE = w_key_rope.shape[1]
    half = ROPE // 2
    context = cache_latent.shape[1] * K
    angle = context * THETA ** (-np.arange(half, dtype=np.float64) / half)
    cos = np.tile(np.cos(angle), 2 * HD)[None].astype(np.float32)
    sin = np.tile(np.concatenate([-np.sin(angle), np.sin(angle)]), HD)[None].astype(np.float32)
    B = R * T
    H = HD * T
    QN, QR, FD = w_query_nope.shape[1], w_query_rope.shape[1], w_gate.shape[1]
    HV = HD * value_up.shape[2]
    big = (w_query_nope, w_query_rope, w_latent, key_turned, key_flat, value_flat, w_out,
           gate_turned, up_turned, w_down, cache_latent, rope_turned)

    def held(a):
        return pltpu.VMEM((ROPE, W) if a is key_turned else a.shape, a.dtype)

    def bf(*shape):
        return pltpu.VMEM(shape, BF16)

    def fl(*shape):
        return pltpu.VMEM(shape, F32)

    LW = LAT + 128
    slabs = fl(W // 128, B, 128)
    gains = pltpu.VMEM((W // 128, 128), BF16)
    scratch = [
        gains, bf(LAT // 128, 128), gains, gains, fl(*cos.shape), fl(*sin.shape),
    ] + [held(a) for a in big] + [
        bf(T, R, W), slabs, bf(K, T, QN + QR), bf(K, T, QN + QR), fl(K, T, 128), fl(K, T, 128),
        fl(R, LW), fl(K, R, LW), bf(T, HD, LW), bf(K, T, HD, LW), bf(K - 1, H, LAT), bf(K, H, LAT),
        fl(K - 1, 8, 2 * H), fl(K, 8, 2 * H), fl(R, LAT), fl(R, 128), bf(T, HD, LAT), bf(T, HD, LAT),
        fl(T, HV), bf(K, T, HV), bf(K, T, W), bf(T, T, W), bf(K, T, W), slabs, slabs,
        bf(K, 2, T, FD), bf(K, 2, T, FD), fl(2, T, FD), bf(K, 2, T, FD), bf(K, 2, T, FD),
        fl(K, T, 128), fl(K, T, 128), bf(K, T, FD), fl(K, T, 128), bf(T, R, W), bf(T, R, W),
        fl(*key_flat.shape), bf(LAT, QN), bf(LAT, HV),
    ]
    vmem = pl.BlockSpec(memory_space=pltpu.VMEM)
    hbm = pl.BlockSpec(memory_space=pl.ANY)
    out_shape = (
        jax.ShapeDtypeStruct((R, W), BF16),
        jax.ShapeDtypeStruct((R, LAT), BF16),
        jax.ShapeDtypeStruct((R, ROPE), BF16),
    )
    made = pl.pallas_call(
        functools.partial(layer_kernel, K, T),
        out_shape=out_shape,
        in_specs=[hbm] * (7 + len(big)),
        out_specs=(vmem, vmem, vmem),
        scratch_shapes=scratch + [
            pltpu.SemaphoreType.DMA((7 + len(big),)),
            pltpu.SemaphoreType.DMA((len(PHASES),)),
            pltpu.SemaphoreType.DMA((len(PHASES),)),
            pltpu.SemaphoreType.DMA((T,)),
            pltpu.SemaphoreType.DMA((K - 1,)),
        ],
        compiler_params=pltpu.CompilerParams(
            collective_id=0, has_side_effects=True, vmem_limit_bytes=60 * 1024 * 1024
        ),
    )(
        resid, *(g.reshape(-1, 128) for g in (attn_gain, latent_gain, post_gain, mlp_gain)),
        jnp.asarray(cos), jnp.asarray(sin), *big,
    )
    return pl.pallas_call(
        hand_over, out_shape=out_shape, in_specs=[vmem] * 3, out_specs=(vmem,) * 3
    )(*made)


def layer(*args):
    resid, key_up = args[0], args[7]
    kv, tp = lax.axis_size("kv"), lax.axis_size("tp")
    if kv == 4 and resid.shape[0] == 4 and key_up.shape[1] == 8 and tp == 8 and resid.shape[1] % 128 == 0:
        return fused(*args)
    return body(*args)


def solution(mesh):
    return jax.shard_map(
        layer,
        mesh=mesh,
        in_specs=(
            P("tp", "kv"),
            P(),
            P("kv", "tp"),
            P("kv", "tp"),
            P("kv", None),
            P(),
            P(),
            P(None, "tp", None),
            P(None, "tp", None),
            P("tp", "kv"),
            P(),
            P(),
            P("kv", "tp"),
            P("kv", "tp"),
            P("tp", "kv"),
            P("tp", "kv", None),
            P("tp", "kv", None),
        ),
        out_specs=(P("tp", "kv"), P("tp", None), P("tp", None)),
        check_vma=False,
    )
```

```python
import functools

import jax
import jax.numpy as jnp
import numpy as np
from jax import lax
from jax.experimental import pallas as pl
from jax.experimental.pallas import tpu as pltpu
from jax.sharding import PartitionSpec as P

EPS = 1e-06
THETA = 10000.0


def rotate(vector, position):
    half_width = vector.shape[-1] // 2
    frequency = THETA ** (-jnp.arange(half_width, dtype=jnp.float32) / half_width)
    angles = jnp.asarray(position, jnp.float32) * frequency
    cos_table, sin_table = (jnp.cos(angles), jnp.sin(angles))
    lower_half, upper_half = (vector[..., :half_width], vector[..., half_width:])
    return jnp.concatenate(
        [
            lower_half * cos_table - upper_half * sin_table,
            lower_half * sin_table + upper_half * cos_table,
        ],
        axis=-1,
    )


def body(
    resid,
    attn_gain,
    w_query_nope,
    w_query_rope,
    w_latent,
    w_key_rope,
    latent_gain,
    key_up,
    value_up,
    w_out,
    post_gain,
    mlp_gain,
    w_gate,
    w_up,
    w_down,
    cache_latent,
    cache_rope_key,
):
    kv_count = lax.axis_size("kv")
    kv_index = lax.axis_index("kv")
    tp_index = lax.axis_index("tp")
    own_rows, width_dev = resid.shape
    model_width = width_dev * kv_count
    heads_dev = key_up.shape[1]
    pos_dev = cache_latent.shape[1]
    context = pos_dev * kv_count
    score_scale = (key_up.shape[2] + cache_rope_key.shape[2]) ** (-0.5)
    col_start = kv_index * width_dev
    row_start = tp_index * own_rows

    def block_of(vector):
        return lax.dynamic_slice_in_dim(vector, col_start, width_dev, 0).astype(jnp.float32)[
            None, :
        ]

    gathered = lax.all_gather(resid, "tp", axis=0, tiled=True)
    batch_rows = gathered.shape[0]
    gathered_float = gathered.astype(jnp.float32)
    normed_a = (gathered_float * block_of(attn_gain)).astype(jnp.bfloat16)
    own_normed = lax.dynamic_slice_in_dim(normed_a, row_start, own_rows, 0)
    key_rows = lax.dynamic_slice_in_dim(w_key_rope, col_start, width_dev, 0)
    q_nope_sum, q_rope_sum, latent_sum, key_sum, square_sum = (
        lax.psum(
            jnp.dot(normed_a, w_query_nope, preferred_element_type=jnp.float32).astype(
                jnp.bfloat16
            ),
            "kv",
        ).astype(jnp.float32),
        lax.psum(
            jnp.dot(normed_a, w_query_rope, preferred_element_type=jnp.float32).astype(
                jnp.bfloat16
            ),
            "kv",
        ).astype(jnp.float32),
        lax.psum(
            jnp.dot(own_normed, w_latent, preferred_element_type=jnp.float32).astype(jnp.bfloat16),
            "kv",
        ).astype(jnp.float32),
        lax.psum(
            jnp.dot(own_normed, key_rows, preferred_element_type=jnp.float32).astype(jnp.bfloat16),
            "kv",
        ).astype(jnp.float32),
        lax.psum(
            jnp.sum(gathered_float * gathered_float, axis=1).astype(jnp.bfloat16), "kv"
        ).astype(jnp.float32),
    )
    scale_in = lax.rsqrt(square_sum / model_width + EPS)[:, None]
    own_scale = lax.dynamic_slice_in_dim(scale_in, row_start, own_rows, 0)
    q_nope = (q_nope_sum * scale_in).astype(jnp.bfloat16).reshape(batch_rows, heads_dev, -1)
    q_rope = rotate((q_rope_sum * scale_in).reshape(batch_rows, heads_dev, -1), context).astype(
        jnp.bfloat16
    )
    new_latent = (
        latent_sum
        * lax.rsqrt(jnp.mean(latent_sum * latent_sum, axis=1, keepdims=True) + EPS)
        * latent_gain.astype(jnp.float32)[None, :]
    ).astype(jnp.bfloat16)
    new_rope_key = rotate(key_sum * own_scale, context).astype(jnp.bfloat16)
    q_lat = jnp.einsum("bhd,chd->bhc", q_nope, key_up, preferred_element_type=jnp.float32).astype(
        jnp.bfloat16
    )
    seq_lat, seq_rope = (
        lax.all_to_all(q_lat, "tp", split_axis=0, concat_axis=1, tiled=True),
        lax.all_to_all(q_rope, "tp", split_axis=0, concat_axis=1, tiled=True),
    )
    scores = (
        jnp.einsum("bhc,bpc->bhp", seq_lat, cache_latent, preferred_element_type=jnp.float32)
        + jnp.einsum("bhr,bpr->bhp", seq_rope, cache_rope_key, preferred_element_type=jnp.float32)
    ) * score_scale
    own_score = (
        jnp.einsum("bhc,bc->bh", seq_lat, new_latent, preferred_element_type=jnp.float32)
        + jnp.einsum("bhr,br->bh", seq_rope, new_rope_key, preferred_element_type=jnp.float32)
    ) * score_scale
    local_peak = jnp.maximum(jnp.max(scores, axis=2), own_score)
    peak = lax.pmax(local_peak, "kv")
    probs = jnp.exp(scores - peak[:, :, None])
    own_prob = jnp.exp(own_score - peak)
    totals = lax.psum(jnp.sum(probs, axis=2), "kv") + own_prob
    partial_value = jnp.einsum(
        "bhp,bpc->bhc", probs.astype(jnp.bfloat16), cache_latent, preferred_element_type=jnp.float32
    )
    summed = (
        lax.psum(partial_value.astype(jnp.bfloat16), "kv").astype(jnp.float32)
        + own_prob[:, :, None] * new_latent.astype(jnp.float32)[:, None, :]
    )
    o_lat = (summed / totals[:, :, None]).astype(jnp.bfloat16)
    head_lat = lax.all_to_all(o_lat, "tp", split_axis=1, concat_axis=0, tiled=True)
    o_heads = jnp.einsum(
        "bhc,che->bhe", head_lat, value_up, preferred_element_type=jnp.float32
    ).astype(jnp.bfloat16)
    o_flat = o_heads.reshape(batch_rows, -1)
    attended = lax.psum_scatter(
        jnp.dot(o_flat, w_out, preferred_element_type=jnp.float32).astype(jnp.bfloat16),
        "tp",
        scatter_dimension=0,
        tiled=True,
    ).astype(jnp.float32)
    post_square = lax.psum(jnp.sum(attended * attended, axis=1), "kv")
    post_part = attended * lax.rsqrt(post_square / model_width + EPS)[:, None] * block_of(post_gain)
    resid_mid = (resid.astype(jnp.float32) + post_part).astype(jnp.bfloat16)
    mid_rows = lax.all_gather(resid_mid, "tp", axis=0, tiled=True)
    mid_float = mid_rows.astype(jnp.float32)
    normed_m = (mid_float * block_of(mlp_gain)).astype(jnp.bfloat16)
    gate_part = jnp.dot(normed_m, w_gate, preferred_element_type=jnp.float32)
    up_part = jnp.dot(normed_m, w_up, preferred_element_type=jnp.float32)
    square_part = jnp.sum(mid_float * mid_float, axis=1)
    gate_sum, up_sum, mid_square = (
        lax.psum(gate_part.astype(jnp.bfloat16), "kv").astype(jnp.float32),
        lax.psum(up_part.astype(jnp.bfloat16), "kv").astype(jnp.float32),
        lax.psum(square_part.astype(jnp.bfloat16), "kv").astype(jnp.float32),
    )
    scale_mid = lax.rsqrt(mid_square / model_width + EPS)[:, None]
    hidden = (jax.nn.silu(gate_sum * scale_mid) * (up_sum * scale_mid)).astype(jnp.bfloat16)
    lowered = lax.psum_scatter(
        jnp.dot(hidden, w_down, preferred_element_type=jnp.float32).astype(jnp.bfloat16),
        "tp",
        scatter_dimension=0,
        tiled=True,
    ).astype(jnp.float32)
    next_resid = (resid_mid.astype(jnp.float32) + lowered).astype(jnp.bfloat16)
    return (next_resid, new_latent, new_rope_key)


F32 = jnp.float32
BF16 = jnp.bfloat16
MESH = pl.DeviceIdType.MESH


def dot_nt(a, b):
    return lax.dot_general(a, b, (((1,), (1,)), ((), ())), preferred_element_type=F32)


def lane_iota(shape):
    return lax.broadcasted_iota(jnp.int32, shape, len(shape) - 1)


def turn(v, cos, sin, half):
    width = v.shape[-1]
    low = lane_iota(v.shape) % (2 * half) < half
    swapped = jnp.where(low, pltpu.roll(v, width - half, 1), pltpu.roll(v, half, 1))
    return v * cos + swapped * sin


def flip(i, mask):
    out, bit = i, 1
    while bit <= mask:
        if mask & bit:
            out = out + bit - 2 * bit * lax.rem(lax.div(i, bit), 2)
        bit *= 2
    return out


PHASES = ("x", "lat", "q", "sq", "qe", "rel", "acc", "ml", "o", "early", "h", "es", "ab", "gu", "sm", "hb", "ps", "ls")


def layer_kernel(
    K, T,
    h_x, h_ag, h_lg, h_pg, h_mg, h_cos, h_sin,
    h_wqn, h_wqr, h_wlat, h_wkr, h_ku, h_vu, h_wo, h_wg, h_wu, h_wd, h_cl, h_cr,
    out, out_lat, out_key,
    ag, lg, pg, mg, cos_ref, sin_ref,
    wqn, wqr, wlat, wkr, ku, vu, wo, wg, wu, wd, cl, cr,
    xbuf, xf, qs, qrv, sqs, sqr, lats, latr, qe, qbuf, accs, accr, mls, mlr,
    nls, nks, osend, obuf, ohs, h3, es, er, ab, attf, tall,
    eas, ear, easum, gus, gur, sms, smr, hb, psb, ls, lr, wide_ref, kus, vus, wgt, wut, clt,
    lsem, ssem, rsem, qsem, relsem,
):
    k = lax.axis_index("kv")
    t = lax.axis_index("tp")
    _, R, W = xbuf.shape
    D = W * K
    B = R * T
    LAT = h_wlat.shape[1]
    ROPE = h_wkr.shape[0]
    QN = h_wqn.shape[1]
    QR = h_wqr.shape[1]
    HD = QR // ROPE
    NOPE = QN // HD
    H = HD * T
    VD = h_vu.shape[1]
    half = ROPE // 2
    score_scale = (NOPE + ROPE) ** (-0.5)
    col = pl.ds(pl.multiple_of(k * W, 128), W)
    gain_rows = pl.ds(pl.multiple_of(k * (W // 128), W // 128), W // 128)

    z, core = lax.div(t, 2), lax.rem(t, 2)
    middle = lax.rem(lax.div(z + 1, 2), 2)
    two, end = lax.rem(z + 2, 4), 3 - z
    far = middle * two + (1 - middle) * end
    mid = middle * end + (1 - middle) * two
    near = flip(z, 1)
    by_arrival = [flip(t, 1)] + [2 * zz + cc for zz in (near, mid, far) for cc in (core, 1 - core)]
    tps = by_arrival[::-1]
    kvs = [flip(k, m) for m in (3, 1, 2)]

    barrier = pltpu.get_barrier_semaphore()
    for kk, tt in [(kk, t) for kk in kvs] + [(k, tt) for tt in tps]:
        pl.semaphore_signal(barrier, inc=1, device_id=(kk, tt), device_id_type=MESH)

    loads = {}
    pairs = [
        ("x", h_x, xbuf.at[t]), ("ag", h_ag.at[gain_rows], ag), ("lat", h_wlat, wlat),
        ("kr", h_wkr.at[:, col], wkr), ("ku", h_ku, ku), ("qn", h_wqn, wqn), ("qr", h_wqr, wqr),
        ("lg", h_lg, lg), ("cos", h_cos, cos_ref), ("sin", h_sin, sin_ref),
        ("vu", h_vu, vu), ("cl", h_cl, cl), ("cr", h_cr, cr),
        ("mg", h_mg.at[gain_rows], mg), ("pg", h_pg.at[gain_rows], pg),
        ("wg", h_wg, wg), ("wu", h_wu, wu), ("wo", h_wo, wo), ("wd", h_wd, wd),
    ]
    for i, (name, src, dst) in enumerate(pairs):
        loads[name] = pltpu.make_async_copy(src, dst, lsem.at[i])
        loads[name].start()

    def send(phase, src, dst, to, landed=None):
        i = PHASES.index(phase)
        pltpu.make_async_remote_copy(
            src_ref=src, dst_ref=dst, send_sem=ssem.at[i],
            recv_sem=rsem.at[i] if landed is None else landed,
            device_id=to, device_id_type=MESH,
        ).start()

    def settle(ref, sem):
        pltpu.make_async_remote_copy(
            src_ref=ref, dst_ref=ref, send_sem=sem, recv_sem=sem,
            device_id=(k, tps[-1]), device_id_type=MESH,
        ).wait_recv()

    def arrive(phase, ref):
        settle(ref, rsem.at[PHASES.index(phase)])

    def left(phase, ref):
        settle(ref, ssem.at[PHASES.index(phase)])

    def dot(a, b):
        return jnp.dot(a, b[...], preferred_element_type=F32)

    def put_rows(ref, s, v):
        for c in range(ref.shape[0]):
            ref[c, pl.ds(s, R, stride=T), :] = v[:, c * 128:(c + 1) * 128]

    def rows(ref, s):
        return jnp.concatenate(
            [ref[c, pl.ds(s, R, stride=T), :] for c in range(ref.shape[0])], axis=1
        )

    def put_all(ref, v):
        for c in range(ref.shape[0]):
            ref[c] = v[:, c * 128:(c + 1) * 128]

    def all_rows(ref):
        return jnp.concatenate([ref[c] for c in range(ref.shape[0])], axis=1)

    def gain_row(ref):
        g = ref[...].astype(F32)
        return jnp.concatenate([g[i:i + 1] for i in range(g.shape[0])], axis=1)

    def by_head(src, dst, turned=False):
        n = src.shape[1]
        wide_ref[...] = src[...].astype(F32)
        for h in range(HD):
            block = wide_ref[pl.ds(h, LAT, stride=HD), :].astype(BF16)
            if turned:
                dst[h * n:(h + 1) * n, :] = block.T
            else:
                dst[:, h * n:(h + 1) * n] = block

    def turn_over(src, dst):
        for c in range(0, src.shape[1], 128):
            dst[c:c + 128, :] = src[:, c:c + 128].T

    loads["x"].wait()
    pl.semaphore_wait(barrier, len(tps) + len(kvs))
    for tt in tps:
        send("x", xbuf.at[t], xbuf.at[t], (k, tt))
    xo = xbuf[pl.ds(t, 1)][0].astype(F32)
    loads["ag"].wait()
    again = gain_row(ag)
    own_normed = (xo * again).astype(BF16)
    loads["lat"].wait()
    loads["kr"].wait()
    lats[:, :LAT] = dot(own_normed, wlat)
    lats[:, LAT:LAT + ROPE] = dot_nt(own_normed, wkr[...])
    lats[:, LAT + ROPE:] = jnp.broadcast_to(
        jnp.sum(xo * xo, axis=1, keepdims=True), (R, lats.shape[1] - LAT - ROPE)
    )
    latr[pl.ds(k, 1)] = lats[...][None]
    for kk in kvs:
        send("lat", lats, latr.at[k], (kk, t))
    loads["ku"].wait()
    by_head(ku, kus, True)
    arrive("x", xbuf.at[pl.ds(0, T - 1)])
    for s in range(T):
        put_rows(xf, s, xbuf[s].astype(F32))
    x = all_rows(xf)
    normed = (x * again).astype(BF16)
    sqs[...] = jnp.broadcast_to(jnp.sum(x * x, axis=1, keepdims=True), (B, 128)).reshape(K, T, 128)
    for name, w, n, size in (("qn", wqn, 0, QN), ("qr", wqr, QN, QR)):
        part = pl.ds(n, size)
        loads[name].wait()
        qs[:, :, part] = dot(normed, w).reshape(K, T, size).astype(BF16)
        for kk in kvs:
            send("q", qs.at[kk, :, part], qrv.at[k, :, part], (kk, t))
    for kk in kvs:
        send("sq", sqs.at[kk], sqr.at[k], (kk, t))
    qrv[pl.ds(k, 1)] = qs[pl.ds(k, 1)]
    sqr[pl.ds(k, 1)] = sqs[pl.ds(k, 1)]
    loads["vu"].wait()
    by_head(vu, vus)
    for name in ("lg", "cos", "sin"):
        loads[name].wait()
    arrive("lat", latr.at[pl.ds(0, K - 1)])
    lat = sum(latr[s] for s in range(K))
    raw = lat[:, :LAT]
    new_lat = (
        raw * lax.rsqrt(jnp.mean(raw * raw, axis=1, keepdims=True) + EPS) * gain_row(lg)
    ).astype(BF16)
    own_scale = lax.rsqrt(lat[:, LAT + ROPE:LAT + ROPE + 1] / D + EPS)
    tail = lat[:, LAT:]
    turned = turn(tail * own_scale, cos_ref[:, :tail.shape[1]], sin_ref[:, :tail.shape[1]], half)
    new_key = jnp.where(lane_iota(turned.shape) < ROPE, turned, 0.0).astype(BF16)
    out_lat[...] = new_lat
    out_key[...] = new_key[:, :ROPE]
    nls[...] = new_lat.astype(F32)
    nks[...] = new_key.astype(F32)

    loads["cl"].wait()
    for r in range(R):
        turn_over(cl.at[r], clt.at[r])
    arrive("q", qrv.at[pl.ds(0, K - 1)])
    arrive("sq", sqr.at[pl.ds(0, K - 1)])
    q = sum(qrv[s].astype(F32) for s in range(K))
    square = sum(sqr[s] for s in range(K))[:, :1]
    scale = lax.rsqrt(square / D + EPS)
    q_nope = (q[:, :QN] * scale).astype(BF16).astype(F32)
    q_rope = turn(q[:, QN:] * scale, cos_ref[...], sin_ref[...], half).astype(BF16).astype(F32)

    def own_head(width, each):
        shape = (HD, width)
        return lane_iota(shape) // each == lax.broadcasted_iota(jnp.int32, shape, 0)

    def spread(v, each):
        mask = own_head(v.shape[1], each)
        return jnp.concatenate(
            [jnp.where(mask, jnp.broadcast_to(v[i:i + 1], mask.shape), 0.0) for i in range(T)], axis=0
        ).astype(BF16)

    RP = qe.shape[2] - LAT
    fold_shape = (QR, RP)
    fold = (
        lax.broadcasted_iota(jnp.int32, fold_shape, 0) % ROPE == lane_iota(fold_shape)
    ).astype(F32).astype(BF16)
    qe[:, :, LAT:] = jnp.dot(
        spread(q_rope, ROPE), fold, preferred_element_type=F32
    ).reshape(T, HD, RP).astype(BF16)
    qe[:, :, :LAT] = dot(spread(q_nope, NOPE), kus).reshape(T, HD, LAT).astype(BF16)
    for tt in tps:
        send("qe", qe.at[tt], qbuf.at[k, t], (k, tt), qsem.at[t])
    HALF = T // 2
    near_start = HALF * lax.div(t, HALF)
    starts = (near_start, HALF - near_start)
    for i, kk in enumerate(kvs):
        send("rel", qe.at[t], qbuf.at[k, t], (kk, t), relsem.at[0, i])
    qbuf[pl.ds(k, 1), pl.ds(t, 1)] = qe[pl.ds(t, 1)][None]
    for n, tt in enumerate(by_arrival):
        slot = qbuf.at[k, tt]
        settle(slot, qsem.at[tt])
        for i, kk in enumerate(kvs):
            send("rel", slot, slot, (kk, t), relsem.at[int(n >= HALF - 1), i])
    loads["cr"].wait()

    def as_row(v, shift):
        shape = (v.shape[0], 2 * H)
        at = lax.broadcasted_iota(jnp.int32, shape, 0) + shift
        return jnp.sum(jnp.where(lane_iota(shape) % H == at, v, 0.0), axis=0, keepdims=True)

    def attend(blocks, start, count):
        wide_qs = [
            qbuf[pl.ds(b, 1), pl.ds(start, count)][0].astype(F32).reshape(count * HD, LAT + RP)
            for b in blocks
        ]
        narrow = [q32.astype(BF16) for q32 in wide_qs]
        scores = [
            (
                jnp.dot(q16[:, :LAT], clt[pl.ds(b, 1)][0], preferred_element_type=F32)
                + jnp.dot(q16[:, LAT:LAT + ROPE], cr[pl.ds(b, 1)][0], preferred_element_type=F32)
            ) * score_scale
            for q16, b in zip(narrow, blocks)
        ]
        tops = [jnp.max(v, axis=1, keepdims=True) for v in scores]
        probs = [jnp.exp(v - m) for v, m in zip(scores, tops)]
        accs_of = [
            jnp.dot(p.astype(BF16), cl[pl.ds(b, 1)][0], preferred_element_type=F32).astype(BF16)
            for p, b in zip(probs, blocks)
        ]
        lanes = lane_iota((count * HD, 2 * H))
        ml_rows = [
            as_row(jnp.where(lanes < H, m, jnp.sum(p, axis=1, keepdims=True)), start * HD)
            for m, p in zip(tops, probs)
        ]
        return wide_qs, accs_of, ml_rows

    (own_qb,), (acc,), (ml,) = attend([k], 0, T)
    accr[pl.ds(k, 1)] = acc[None]
    mlr[pl.ds(k, 1), 0, 0:1, :] = ml[None]
    mlr[pl.ds(k, 1), 1, 0:1, :] = jnp.zeros_like(ml)[None]
    nl = nls[pl.ds(k, 1), :]
    nk = nks[pl.ds(k, 1), :]
    own_score = as_row((
        jnp.sum(own_qb[:, :LAT] * nl, axis=1, keepdims=True)
        + jnp.sum(own_qb[:, LAT:] * nk, axis=1, keepdims=True)
    ) * score_scale, 0)
    for part, start in enumerate(starts):
        for i, kk in enumerate(kvs):
            settle(qbuf.at[kk, pl.ds(start, HALF)], relsem.at[part, i])
        _, part_accs, part_mls = attend(kvs, start, HALF)
        heads = pl.ds(pl.multiple_of(start * HD, HALF * HD), HALF * HD)
        for i, kk in enumerate(kvs):
            mls[i, part, 0:1, :] = part_mls[i]
            send("ml", mls.at[i, part], mlr.at[k, part], (kk, t))
        for i, kk in enumerate(kvs):
            accs[i, part] = part_accs[i]
            send("acc", accs.at[i, part], accr.at[k, heads], (kk, t))
    arrive("ml", mlr.at[pl.ds(0, K - 1)])
    peaks = jnp.concatenate([mlr[s, 0, 0:1, :] + mlr[s, 1, 0:1, :] for s in range(K)], axis=0)
    peak = jnp.maximum(jnp.max(peaks, axis=0, keepdims=True), own_score)
    share = jnp.exp(peaks - peak)
    own_prob = jnp.exp(own_score - peak)
    total = own_prob + jnp.sum(share * pltpu.roll(peaks, H, 1), axis=0, keepdims=True)
    own_share = jnp.broadcast_to(own_prob / total, (8 - K, 2 * H))
    columns = jnp.concatenate([share / total, own_share], axis=0).T[:H]
    arrive("acc", accr.at[pl.ds(0, K - 1)])
    summed = columns[:, K:K + 1] * nl
    for s in range(K):
        summed = summed + columns[:, s:s + 1] * accr[s].astype(F32)
    osend[...] = summed.reshape(T, HD, LAT).astype(BF16)
    for tt in tps:
        send("o", osend.at[tt], obuf.at[t], (k, tt))
    obuf[pl.ds(t, 1)] = osend[pl.ds(t, 1)]

    FD = wg.shape[0]
    loads["mg"].wait()
    early = (all_rows(xf) * gain_row(mg)).astype(BF16)
    for i, (name, w) in enumerate((("wg", wg), ("wu", wu))):
        loads[name].wait()
        eas[:, i] = dot_nt(early, w[...]).reshape(K, T, FD).astype(BF16)
        for kk in kvs:
            send("early", eas.at[kk, i], ear.at[k, i], (kk, t))
    ear[pl.ds(k, 1)] = eas[pl.ds(k, 1)]
    arrive("o", obuf.at[pl.ds(0, T - 1)])
    wide = dot(obuf[...].astype(F32).reshape(T * HD, LAT).astype(BF16), vus)
    mask = own_head(HD * VD, VD)
    for i in range(T):
        ohs[i:i + 1, :] = jnp.sum(
            jnp.where(mask, wide[i * HD:(i + 1) * HD], 0.0), axis=0, keepdims=True
        )
    h3[pl.ds(k, 1)] = ohs[...].astype(BF16)[None]
    for kk in kvs:
        send("h", h3.at[k], h3.at[k], (kk, t))
    turn_over(wu, wut)
    loads["wo"].wait()
    arrive("h", h3.at[pl.ds(0, K - 1)])
    OWNERS, share_rows = es.shape[0], es.shape[1]
    es[...] = dot(
        h3[...].astype(F32).reshape(B, HD * VD).astype(BF16), wo
    ).reshape(OWNERS, share_rows, W).astype(BF16)
    owners = (T // 2 - 1, T // 2 + 1)
    mine = lax.div(t, T // 2)
    owner = lax.rem(t + 1, T) == mine * 2 + T // 2
    for i in range(OWNERS):
        j = lax.rem(i + 1 + mine, OWNERS)

        @pl.when(jnp.logical_not(jnp.logical_and(owner, mine == j)))
        def _():
            send("es", es.at[j], er.at[t], (k, 2 * j + owners[0]))

    turn_over(wg, wgt)
    arrive("early", ear.at[pl.ds(0, K - 1)])
    easum[...] = sum(ear[s].astype(F32) for s in range(K))
    loads["pg"].wait()

    @pl.when(owner)
    def _():
        er[pl.ds(t, 1)] = es[pl.ds(mine, 1)]
        arrive("es", er.at[pl.ds(0, T - 1)])
        ab[pl.ds(mine, 1)] = sum(er[s].astype(F32) for s in range(T)).astype(BF16)[None]
        for tt in tps:
            send("ab", ab.at[mine], ab.at[mine], (k, tt))
        arrive("ab", ab.at[pl.ds(0, OWNERS - 1)])

    @pl.when(jnp.logical_not(owner))
    def _():
        arrive("ab", ab)

    att = ab[...].astype(F32).reshape(B, W)
    added = att * gain_row(pg)
    late = (added * gain_row(mg)).astype(BF16)
    lane = lane_iota((B, 128))
    parts = (
        jnp.sum(att * att, axis=1, keepdims=True),
        jnp.sum(all_rows(xf) * added, axis=1, keepdims=True),
        jnp.sum(added * added, axis=1, keepdims=True),
    )
    sms[...] = jnp.where(
        lane < 32, parts[0], jnp.where(lane < 64, parts[1], parts[2])
    ).reshape(K, T, 128)
    cut = (FD // 256 + 1) * 128
    for i, w, n, size in ((0, wgt, 0, FD), (1, wut, 0, cut), (1, wut, cut, FD - cut)):
        part = pl.ds(n, size)
        gus[:, i, :, part] = dot(late, w.at[:, part]).reshape(K, T, size).astype(BF16)
        for kk in kvs:
            send("gu", gus.at[kk, i, :, part], gur.at[k, i, :, part], (kk, t))
        if i == 0:
            for kk in kvs:
                send("sm", sms.at[kk], smr.at[k], (kk, t))
    gur[pl.ds(k, 1)] = gus[pl.ds(k, 1)]
    smr[pl.ds(k, 1)] = sms[pl.ds(k, 1)]
    put_all(attf, att)
    arrive("sm", smr.at[pl.ds(0, K - 1)])
    sums = sum(smr[s] for s in range(K))
    post_scale = lax.rsqrt(sums[:, :1] / D + EPS)
    mid_square = square + post_scale * (2.0 * sums[:, 32:33] + post_scale * sums[:, 64:65])
    mid_scale = lax.rsqrt(jnp.maximum(mid_square, 0.0) / D + EPS)
    arrive("gu", gur.at[pl.ds(0, K - 1)])
    gate = (easum[0] + post_scale * sum(gur[s, 0].astype(F32) for s in range(K))) * mid_scale
    up = (easum[1] + post_scale * sum(gur[s, 1].astype(F32) for s in range(K))) * mid_scale
    hb[pl.ds(k, 1)] = (gate / (1.0 + jnp.exp(-gate)) * up).astype(BF16)[None]
    psb[pl.ds(k, 1)] = jnp.broadcast_to(post_scale, (T, 128))[None]
    for kk in kvs:
        send("hb", hb.at[k], hb.at[k], (kk, t))
        send("ps", psb.at[k], psb.at[k], (kk, t))
    loads["wd"].wait()
    arrive("hb", hb.at[pl.ds(0, K - 1)])
    put_all(tall, dot(hb[...].astype(F32).reshape(B, FD).astype(BF16), wd))
    for s in range(T):
        ls[s] = rows(tall, s).astype(BF16)
    for tt in tps:
        send("ls", ls.at[tt], lr.at[t], (k, tt))
    lr[pl.ds(t, 1)] = ls[pl.ds(t, 1)]
    arrive("ps", psb.at[pl.ds(0, K - 1)])
    own_post = psb[:, pl.ds(t, 1), :].reshape(K, 128)[:, :1]
    mid_own = (
        xbuf[pl.ds(t, 1)][0].astype(F32) + rows(attf, t) * own_post * gain_row(pg)
    ).astype(BF16).astype(F32)
    left("x", xbuf.at[pl.ds(0, T - 1)])
    left("lat", latr.at[pl.ds(0, K - 1)])
    left("q", qs.at[pl.ds(0, K - 1)])
    left("sq", sqs.at[pl.ds(0, K - 1)])
    left("qe", qe.at[pl.ds(0, T - 1)])
    left("rel", qbuf.at[pl.ds(0, K - 1)])
    left("acc", accs)
    left("ml", mls)
    left("o", osend.at[pl.ds(0, T - 1)])
    left("early", eas.at[pl.ds(0, K - 1)])
    left("h", h3.at[pl.ds(0, K - 1)])

    @pl.when(owner)
    def _():
        left("es", es.at[pl.ds(0, OWNERS - 1)])
        left("ab", er.at[pl.ds(0, T - 1)])

    @pl.when(jnp.logical_not(owner))
    def _():
        left("es", es)

    left("gu", gus.at[pl.ds(0, K - 1)])
    left("sm", sms.at[pl.ds(0, K - 1)])
    left("hb", hb.at[pl.ds(0, K - 1)])
    left("ps", psb.at[pl.ds(0, K - 1)])
    arrive("ls", lr.at[pl.ds(0, T - 1)])
    lowered = sum(lr[s].astype(F32) for s in range(T))
    out[...] = (mid_own + lowered).astype(BF16)
    left("ls", ls.at[pl.ds(0, T - 1)])


def hand_over(a, b, c, a_out, b_out, c_out):
    for src, dst in ((a, a_out), (b, b_out), (c, c_out)):
        dst[...] = src[...]


def fused(
    resid, attn_gain, w_query_nope, w_query_rope, w_latent, w_key_rope, latent_gain, key_up,
    value_up, w_out, post_gain, mlp_gain, w_gate, w_up, w_down, cache_latent, cache_rope_key,
):
    K = lax.axis_size("kv")
    T = lax.axis_size("tp")
    R, W = resid.shape
    LAT, HD, _ = key_up.shape
    key_flat = key_up.reshape(LAT * HD, -1)
    value_flat = value_up.reshape(LAT * HD, -1)
    key_turned, rope_turned = w_key_rope.T, jnp.swapaxes(cache_rope_key, 1, 2)
    gate_turned, up_turned = w_gate.T, w_up.T
    ROPE = w_key_rope.shape[1]
    half = ROPE // 2
    context = cache_latent.shape[1] * K
    angle = context * THETA ** (-np.arange(half, dtype=np.float64) / half)
    cos = np.tile(np.cos(angle), 2 * HD)[None].astype(np.float32)
    sin = np.tile(np.concatenate([-np.sin(angle), np.sin(angle)]), HD)[None].astype(np.float32)
    B = R * T
    H = HD * T
    QN, QR, FD = w_query_nope.shape[1], w_query_rope.shape[1], w_gate.shape[1]
    HV = HD * value_up.shape[2]
    big = (w_query_nope, w_query_rope, w_latent, key_turned, key_flat, value_flat, w_out,
           gate_turned, up_turned, w_down, cache_latent, rope_turned)

    def held(a):
        return pltpu.VMEM((ROPE, W) if a is key_turned else a.shape, a.dtype)

    def bf(*shape):
        return pltpu.VMEM(shape, BF16)

    def fl(*shape):
        return pltpu.VMEM(shape, F32)

    LW = LAT + 128
    slabs = fl(W // 128, B, 128)
    gains = pltpu.VMEM((W // 128, 128), BF16)
    scratch = [
        gains, bf(LAT // 128, 128), gains, gains, fl(*cos.shape), fl(*sin.shape),
    ] + [held(a) for a in big] + [
        bf(T, R, W), slabs, bf(K, T, QN + QR), bf(K, T, QN + QR), fl(K, T, 128), fl(K, T, 128),
        fl(R, LW), fl(K, R, LW), bf(T, HD, LW), bf(K, T, HD, LW), bf(K - 1, 2, H // 2, LAT), bf(K, H, LAT),
        fl(K - 1, 2, 8, 2 * H), fl(K, 2, 8, 2 * H), fl(R, LAT), fl(R, 128), bf(T, HD, LAT), bf(T, HD, LAT),
        fl(T, HV), bf(K, T, HV), bf(2, B // 2, W), bf(T, B // 2, W), bf(2, B // 2, W), slabs, slabs,
        bf(K, 2, T, FD), bf(K, 2, T, FD), fl(2, T, FD), bf(K, 2, T, FD), bf(K, 2, T, FD),
        fl(K, T, 128), fl(K, T, 128), bf(K, T, FD), fl(K, T, 128), bf(T, R, W), bf(T, R, W),
        fl(*key_flat.shape), bf(QN, LAT), bf(LAT, HV), bf(W, FD), bf(W, FD),
        bf(R, LAT, cache_latent.shape[1]),
    ]
    vmem = pl.BlockSpec(memory_space=pltpu.VMEM)
    hbm = pl.BlockSpec(memory_space=pltpu.HBM)
    shapes = ((R, W), (R, LAT), (R, ROPE))
    made = pl.pallas_call(
        functools.partial(layer_kernel, K, T),
        out_shape=tuple(pltpu.VMEM(shape, BF16) for shape in shapes),
        in_specs=[hbm] * (7 + len(big)),
        out_specs=(vmem, vmem, vmem),
        scratch_shapes=scratch + [
            pltpu.SemaphoreType.DMA((7 + len(big),)),
            pltpu.SemaphoreType.DMA((len(PHASES),)),
            pltpu.SemaphoreType.DMA((len(PHASES),)),
            pltpu.SemaphoreType.DMA((T,)),
            pltpu.SemaphoreType.DMA((2, K - 1)),
        ],
        compiler_params=pltpu.CompilerParams(
            collective_id=0, has_side_effects=True, vmem_limit_bytes=60 * 1024 * 1024
        ),
    )(
        resid, *(g.reshape(-1, 128) for g in (attn_gain, latent_gain, post_gain, mlp_gain)),
        jnp.asarray(cos), jnp.asarray(sin), *big,
    )
    return pl.pallas_call(
        hand_over,
        out_shape=tuple(jax.ShapeDtypeStruct(shape, BF16) for shape in shapes),
        in_specs=[vmem] * 3,
        out_specs=(vmem,) * 3,
    )(*(pltpu.with_memory_space_constraint(a, pltpu.VMEM) for a in made))


def layer(*args):
    resid, key_up = args[0], args[7]
    kv, tp = lax.axis_size("kv"), lax.axis_size("tp")
    if kv == 4 and resid.shape[0] == 4 and key_up.shape[1] == 8 and tp == 8 and resid.shape[1] % 128 == 0:
        return fused(*args)
    return body(*args)


def solution(mesh):
    return jax.shard_map(
        layer,
        mesh=mesh,
        in_specs=(
            P("tp", "kv"),
            P(),
            P("kv", "tp"),
            P("kv", "tp"),
            P("kv", None),
            P(),
            P(),
            P(None, "tp", None),
            P(None, "tp", None),
            P("tp", "kv"),
            P(),
            P(),
            P("kv", "tp"),
            P("kv", "tp"),
            P("tp", "kv"),
            P("tp", "kv", None),
            P("tp", "kv", None),
        ),
        out_specs=(P("tp", "kv"), P("tp", None), P("tp", None)),
        check_vma=False,
    )
```
